32 devices in a mesh: rep: 2 (over x), fs: 8 (over z, y), tp: 2 (over core).
Axes of the slice: x: 2, y: 2, z: 4, core: 2. Of those that a mesh axis runs over, the one named last changes fastest.
Arguments:
- tokens: bfloat16 [12288, 2048], P(('rep', 'fs', 'tp')), may hold values from -6 to 6
- outer_weight: float32 [2048, 1536], P('fs', 'tp'), may hold values from -0.125 to 0.125
- inner_weight: float32 [2048, 1536], P('fs', 'tp'), may hold values from -0.125 to 0.125
- value_weight: float32 [2048, 1536], P('fs', 'tp'), may hold values from -0.125 to 0.125
- conv_taps: float32 [3, 1536], P(None, 'tp'), may hold values from -3 to 3
- mix_out: float32 [1536, 2048], P('tp', 'fs'), may hold values from -0.15625 to 0.15625
- norm_first: float32 [2048], replicated, may hold values from 0.1 to 1.9
- up_weight: float32 [2048, 4096], P('fs', 'tp'), may hold values from -0.125 to 0.125
- down_weight: float32 [4096, 2048], P('tp', 'fs'), may hold values from -0.09375 to 0.09375
- norm_second: float32 [2048], replicated, may hold values from 0.1 to 1.9
Outputs:
- encoded: bfloat16 [12288, 2048], P(('rep', 'fs', 'tp'))
The draws below stay inside these ranges and needn't reach their ends.
All inputs are finite; a program needn't handle non-finite values.
Results may differ from the reference program's by a relative error of at most 0.015.
Values may be sent and summed in bfloat16 or wider, within the bound.
A program may use at most 128 MiB of HBM per device.

```python
import jax
import jax.numpy as jnp
from jax import lax

D = 2048
WA = 1536
FF = 4096
SEQ = 128
TOK_DEV = 384
TOKENS = 12288


def level_of(own_key, dims, split, least, top_value):
    gain, own = 1.0, jax.random.fold_in(own_key, 6)
    for axis_at, parts in split:
        steps = jnp.exp(jax.random.uniform(jax.random.fold_in(own, axis_at), (parts,), jnp.float32, least / len(split), top_value / len(split)))
        gain = gain * jnp.repeat(steps, dims[axis_at] // parts).reshape([-1 if axis == axis_at else 1 for axis in range(len(dims))])
    return gain


def gaussian(rng, dims, width, reach, split=(), kind=jnp.bfloat16):
    drawn = jax.random.normal(rng, dims, jnp.float32) * width
    if len(split) > 0:
        drawn = level_of(rng, dims, split, -0.22, 0.18) * drawn
    return jnp.clip(drawn, min=-reach, max=reach).astype(kind)


def setup_inputs(seed: int = 0) -> dict:
    arg_keys = jax.random.split(jax.random.key(seed), 11)
    tokens = gaussian(arg_keys[0], (TOKENS, D), 1.0, 6.0, ((0, 32),))
    outer_weight = gaussian(arg_keys[1], (D, WA), D ** -0.5, 0.125, ((0, 8), (1, 2)), jnp.float32)
    inner_weight = gaussian(arg_keys[2], (D, WA), D ** -0.5, 0.125, ((0, 8), (1, 2)), jnp.float32)
    value_weight = gaussian(arg_keys[3], (D, WA), D ** -0.5, 0.125, ((0, 8), (1, 2)), jnp.float32)
    conv_taps = gaussian(arg_keys[4], (3, WA), 0.6, 3.0, ((1, 2),), jnp.float32)
    mix_out = gaussian(arg_keys[5], (WA, D), WA ** -0.5, 0.15625, ((0, 2), (1, 8)), jnp.float32)
    norm_first = jnp.clip(1.0 + 0.18 * jax.random.normal(arg_keys[6], (D,), jnp.float32), 0.1, 1.9)
    up_weight = gaussian(arg_keys[7], (D, FF), D ** -0.5, 0.125, ((0, 8), (1, 2)), jnp.float32)
    down_weight = gaussian(arg_keys[8], (FF, D), FF ** -0.5, 0.09375, ((0, 2), (1, 8)), jnp.float32)
    norm_second = jnp.clip(1.0 + 0.18 * jax.random.normal(arg_keys[9], (D,), jnp.float32), 0.1, 1.9)
    return {"tokens": tokens, "outer_weight": outer_weight, "inner_weight": inner_weight, "value_weight": value_weight, "conv_taps": conv_taps, "mix_out": mix_out, "norm_first": norm_first, "up_weight": up_weight, "down_weight": down_weight, "norm_second": norm_second}


residual_scale = 2.0 ** 0.25
norm_epsilon = 1e-05

def layer_norm(values, scaling):
    center = values - lax.optimization_barrier(jnp.mean(values, axis=-1, keepdims=True))
    spread = lax.optimization_barrier(jnp.mean(center * center, axis=-1, keepdims=True))
    return center * lax.rsqrt(spread + norm_epsilon) * scaling

def reference(tokens, outer_weight, inner_weight, value_weight, conv_taps, mix_out, norm_first, up_weight, down_weight, norm_second):
    outer_bf = outer_weight.astype(jnp.bfloat16)
    inner_bf = inner_weight.astype(jnp.bfloat16)
    value_bf = value_weight.astype(jnp.bfloat16)
    mixout_bf = mix_out.astype(jnp.bfloat16)
    upward_bf = up_weight.astype(jnp.bfloat16)
    downward_bf = down_weight.astype(jnp.bfloat16)
    blocks = tokens.reshape(-1, TOK_DEV * 8, D)

    def one_block(rows):
        outer = jnp.dot(rows, outer_bf, preferred_element_type=jnp.float32)
        inner = jnp.dot(rows, inner_bf, preferred_element_type=jnp.float32)
        value = jnp.dot(rows, value_bf, preferred_element_type=jnp.float32)
        framed = (inner * value).reshape(-1, SEQ, WA)
        padded = jnp.pad(framed, ((0, 0), (1, 1), (0, 0)))
        convolved = padded[:, :-2] * conv_taps[0] + framed * conv_taps[1] + padded[:, 2:] * conv_taps[2]
        mixed = (outer * convolved.reshape(-1, WA)).astype(jnp.bfloat16)
        mixing = jnp.dot(mixed, mixout_bf, preferred_element_type=jnp.float32)
        first = layer_norm(residual_scale * rows.astype(jnp.float32) + mixing, norm_first).astype(jnp.bfloat16)
        raised = jax.nn.relu(jnp.dot(first, upward_bf, preferred_element_type=jnp.float32))
        hidden = (raised * raised).astype(jnp.bfloat16)
        lowered = jnp.dot(hidden, downward_bf, preferred_element_type=jnp.float32)
        return layer_norm(residual_scale * first.astype(jnp.float32) + lowered, norm_second).astype(jnp.bfloat16)
    return lax.map(one_block, blocks).reshape(tokens.shape[0], D)
```

```python
import functools

import jax
import jax.numpy as jnp
from jax import lax
from jax.experimental import pallas as pl
from jax.experimental.pallas import tpu as pltpu
from jax.sharding import PartitionSpec as P

SEQ = 128


residual_scale = 2.0**0.25
norm_epsilon = 1e-05


def layer_norm(values, scaling):
    center = values - jnp.mean(values, axis=-1, keepdims=True)
    spread = jnp.mean(center * center, axis=-1, keepdims=True)
    return center * lax.rsqrt(spread + norm_epsilon) * scaling


def short_conv(product, conv_taps):
    places = jnp.arange(product.shape[0], dtype=jnp.int32) % SEQ
    blank = jnp.zeros((1, product.shape[1]), jnp.float32)
    before = jnp.concatenate([blank, product[:-1]], axis=0)
    after = jnp.concatenate([product[1:], blank], axis=0)
    before = jnp.where((places > 0)[:, None], before, 0.0)
    after = jnp.where((places < SEQ - 1)[:, None], after, 0.0)
    return conv_taps[0] * before + conv_taps[1] * product + conv_taps[2] * after


def local(
    tokens,
    outer_weight,
    inner_weight,
    value_weight,
    conv_taps,
    mix_out,
    norm_first,
    up_weight,
    down_weight,
    norm_second,
):
    grouped = lax.all_gather(tokens, "tp", axis=0, tiled=True)
    outer_bf = outer_weight.astype(jnp.bfloat16)
    inner_bf = inner_weight.astype(jnp.bfloat16)
    value_bf = value_weight.astype(jnp.bfloat16)
    outer_full, inner_full, value_full = (
        lax.all_gather(outer_bf, "fs", axis=0, tiled=True),
        lax.all_gather(inner_bf, "fs", axis=0, tiled=True),
        lax.all_gather(value_bf, "fs", axis=0, tiled=True),
    )
    outer = jnp.dot(grouped, outer_full, preferred_element_type=jnp.float32)
    inner = jnp.dot(grouped, inner_full, preferred_element_type=jnp.float32)
    value = jnp.dot(grouped, value_full, preferred_element_type=jnp.float32)
    mixed = (outer * short_conv(inner * value, conv_taps)).astype(jnp.bfloat16)
    mixout_full = lax.all_gather(mix_out.astype(jnp.bfloat16), "fs", axis=1, tiled=True)
    selected = mixed
    mixing = lax.psum_scatter(
        jnp.dot(selected, mixout_full, preferred_element_type=jnp.float32).astype(jnp.bfloat16),
        "tp",
        scatter_dimension=0,
        tiled=True,
    ).astype(jnp.float32)
    first = layer_norm(residual_scale * tokens.astype(jnp.float32) + mixing, norm_first).astype(
        jnp.bfloat16
    )
    grouped_first = lax.all_gather(first, "tp", axis=0, tiled=True)
    upward_bf = up_weight.astype(jnp.bfloat16)
    upward_full = lax.all_gather(upward_bf, "fs", axis=0, tiled=True)
    raised = jnp.dot(grouped_first, upward_full, preferred_element_type=jnp.float32)
    raised = jax.nn.relu(raised)
    hidden = (raised * raised).astype(jnp.bfloat16)
    down_full = lax.all_gather(down_weight.astype(jnp.bfloat16), "fs", axis=1, tiled=True)
    selected = hidden
    lowered = lax.psum_scatter(
        jnp.dot(selected, down_full, preferred_element_type=jnp.float32).astype(jnp.bfloat16),
        "tp",
        scatter_dimension=0,
        tiled=True,
    ).astype(jnp.float32)
    return layer_norm(residual_scale * first.astype(jnp.float32) + lowered, norm_second).astype(
        jnp.bfloat16
    )


MESH = pl.DeviceIdType.MESH
BF = jnp.bfloat16
F32 = jnp.float32


def dot(a, b):
    return jnp.dot(a, b, preferred_element_type=F32)


def third_rows(rows):
    return (rows // 3 + 8) // 16 * 16


def layer_kernel(
    n,
    tokens_hbm,
    outer_hbm,
    inner_hbm,
    value_hbm,
    taps_ref,
    mix_hbm,
    norm1_ref,
    up_hbm,
    down_hbm,
    norm2_ref,
    out_ref,
    wa,
    wb,
    wc,
    wd,
    stage_a,
    stage_b,
    stage_d,
    tok,
    acc,
    mixed,
    own,
    psend,
    precv1,
    precv2,
    fst,
    hid,
    load_sem,
    ring_send,
    ring_recv,
    tp_send,
    tp_recv,
):
    half = n // 2
    r = lax.axis_index("rep")
    f = lax.axis_index("fs")
    t = lax.axis_index("tp")
    rows = tokens_hbm.shape[0]
    both = 2 * rows
    d = tokens_hbm.shape[1]
    ks = wa.shape[2]
    wch = wa.shape[3]
    ff = wc.shape[2]
    nc = wb.shape[2]

    odd = f % 2
    pos = (1 - odd) * (f // 2) + odd * (n - 1 - f // 2)

    def at(place):
        p = (place + 2 * n) % n
        hi = p // half
        return (1 - hi) * (2 * p) + hi * (2 * (n - 1 - p) + 1)

    right = {"fs": at(pos + 1)}
    left = {"fs": at(pos - 1)}
    across = {"rep": 1 - r}
    mate = {"tp": 1 - t}

    loads = [
        pltpu.make_async_copy(outer_hbm, stage_a.at[0], load_sem.at[0]),
        pltpu.make_async_copy(inner_hbm, stage_a.at[1], load_sem.at[1]),
        pltpu.make_async_copy(value_hbm, stage_a.at[2], load_sem.at[2]),
        pltpu.make_async_copy(mix_hbm, stage_b, load_sem.at[3]),
        pltpu.make_async_copy(
            up_hbm, acc.at[pl.ds(0, ks), pl.ds(0, ff)], load_sem.at[4]
        ),
        pltpu.make_async_copy(down_hbm, stage_d, load_sem.at[5]),
        pltpu.make_async_copy(tokens_hbm, tok.at[pl.ds(0, rows)], load_sem.at[6]),
    ]
    for load in loads:
        load.start()

    barrier = pltpu.get_barrier_semaphore()
    for device in (right, left, across, mate):
        pl.semaphore_signal(barrier, inc=1, device_id=device, device_id_type=MESH)
    pl.semaphore_wait(barrier, 4)

    def mate_copy(i, src, dst):
        return pltpu.make_async_remote_copy(
            src_ref=src,
            dst_ref=dst,
            send_sem=tp_send.at[i],
            recv_sem=tp_recv.at[i],
            device_id=mate,
            device_id_type=MESH,
        )

    def piece(ti, which, owner):
        if ti == 0:
            return wa.at[2 if which else r, owner]
        ref = (None, wb, wc, wd)[ti]
        u = third_rows(ref.shape[1])
        if which:
            return ref.at[owner, pl.ds(2 * u, ref.shape[1] - 2 * u)]
        return ref.at[owner, pl.ds(pl.multiple_of(r * u, 16), u)]

    per = 6 * half - 3
    index = {}
    for h in range(1, half + 1):
        for kind in ("Rq", "Rp", "Lq", "Lp", "XR", "XL"):
            if h == half and kind in ("Rp", "Lq", "XL"):
                continue
            index[kind, h] = len(index)

    copies = {}

    def message(ti, kind, h):
        key = (ti, kind, h)
        if key not in copies:
            which = kind[1] == "p"
            if kind[0] == "R":
                src, device = at(pos - (h - 1)), right
            elif kind[0] == "L":
                src, device = at(pos + (h - 1)), left
            else:
                src, device = at(pos - h if kind == "XR" else pos + h), across
            i = ti * per + index[kind, h]
            ref = piece(ti, which, src)
            copies[key] = pltpu.make_async_remote_copy(
                src_ref=ref,
                dst_ref=ref,
                send_sem=ring_send.at[i],
                recv_sem=ring_recv.at[i],
                device_id=device,
                device_id_type=MESH,
            )
        return copies[key]

    def send(ti, kind, h):
        if ti < 4 and (kind, h) in index:
            message(ti, kind, h).start()

    def got(ti, kind, h):
        message(ti, kind, h).wait_recv()

    def event(ti, h, which):
        if which == 0:
            got(ti, "Rq", h)
            send(ti, "Rq", h + 1)
            send(ti, "XR", h)
            if h < half:
                got(ti, "Lq", h)
                if h + 1 < half:
                    send(ti, "Lq", h + 1)
                else:
                    send(ti + 1, "Lq", 1)
                send(ti, "XL", h)
            else:
                send(ti + 1, "Rp", 1)
                got(ti, "Lp", h)
                send(ti + 1, "Lp", 1)
        else:
            got(ti, "Rp", h)
            if h + 1 < half:
                send(ti, "Rp", h + 1)
            else:
                send(ti + 1, "Rq", 1)
            got(ti, "Lp", h)
            send(ti, "Lp", h + 1)

    def events(ti):
        out = []
        for h in range(1, half + 1):
            out.append((ti, h, 0))
            if h < half:
                out.append((ti, h, 1))
        return out

    def arrived(ti, h):
        got(ti, "XR", h)
        if h < half:
            got(ti, "XL", h)

    def owners(h):
        if h == 0:
            return [f]
        if h == half:
            return [at(pos + half)]
        return [at(pos - h), at(pos + h)]

    for i in range(3):
        loads[i].wait()
        wa[i, f] = stage_a[i].astype(BF)
    send(0, "Rq", 1)
    send(0, "Lq", 1)
    send(0, "Rp", 1)
    send(0, "Lp", 1)
    share = mate_copy(0, tokens_hbm, tok.at[pl.ds(rows, rows)])
    share.start()
    loads[3].wait()
    wb[f] = stage_b[...].astype(BF)
    loads[4].wait()
    wc[f] = acc[pl.ds(0, ks), pl.ds(0, ff)].astype(BF)
    loads[5].wait()
    wd[f] = stage_d[...].astype(BF)
    loads[6].wait()
    share.wait_recv()

    tn = 256

    def accumulate(x_ref, h, weight, width, base):
        who = owners(h)

        def unit(i, _):
            m = pl.multiple_of((i % 2) * rows, 16)
            c = pl.multiple_of((i // 2) * tn, tn)
            total = None
            for o in who:
                x = x_ref[pl.ds(m, rows), pl.ds(pl.multiple_of(o * ks, 128), ks)]
                term = dot(x, weight(o, pl.ds(c, tn)))
                total = term if total is None else total + term
            span = pl.ds(pl.multiple_of(base + c, tn), tn)
            if h == 0:
                acc[pl.ds(m, rows), span] = total
            else:
                acc[pl.ds(m, rows), span] += total
            return 0

        lax.fori_loop(0, 2 * (width // tn), unit, 0)

    def project(h):
        for i in range(3):
            accumulate(tok, h, lambda o, c, i=i: wa[i, o, :, c], wch, i * wch)

    def raise_(h):
        accumulate(fst, h, lambda o, c: wc[o, :, c], ff, 0)

    def lower(x_ref, w_ref, h, recv, first_sem):
        for k, o in enumerate(owners(h)):
            psend[o] = dot(x_ref[pl.ds(rows, rows), :], w_ref[o]).astype(BF)
            mate_block(first_sem, h, k, o, recv).start()
            own[o] = dot(x_ref[pl.ds(0, rows), :], w_ref[o])

    def mate_block(first_sem, h, k, o, recv):
        i = first_sem + (0 if h == 0 else 2 * h - 1 + k)
        return mate_copy(i, psend.at[o], recv.at[o])

    def mate_blocks(first_sem, recv):
        return [
            mate_block(first_sem, h, k, o, recv)
            for h in range(half + 1)
            for k, o in enumerate(owners(h))
        ]

    def mix():
        seq = SEQ

        def unit(i, _):
            m = pl.multiple_of((i % (both // seq)) * seq, seq)
            c = pl.multiple_of((i // (both // seq)) * tn, tn)
            o = acc[pl.ds(m, seq), pl.ds(c, tn)]
            p = (
                acc[pl.ds(m, seq), pl.ds(pl.multiple_of(wch + c, tn), tn)]
                * acc[pl.ds(m, seq), pl.ds(pl.multiple_of(2 * wch + c, tn), tn)]
            )
            place = lax.broadcasted_iota(jnp.int32, p.shape, 0)
            before = jnp.where(place > 0, pltpu.roll(p, 1, 0), 0.0)
            after = jnp.where(place < seq - 1, pltpu.roll(p, seq - 1, 0), 0.0)
            taps = taps_ref[:, pl.ds(c, tn)]
            conv = taps[0:1] * before + taps[1:2] * p + taps[2:3] * after
            mixed[pl.ds(m, seq), pl.ds(c, tn)] = (o * conv).astype(BF)
            return 0

        lax.fori_loop(0, (both // seq) * (wch // tn), unit, 0)

    def norm(base_ref, recv, gain_ref, dest_ref):
        tm = 32

        def unit(i, _):
            m = pl.multiple_of(i * tm, tm)
            parts = [
                residual_scale
                * base_ref[pl.ds(m, tm), pl.ds(b * nc, nc)].astype(F32)
                + own[b, pl.ds(m, tm)]
                + recv[b, pl.ds(m, tm)].astype(F32)
                for b in range(n)
            ]
            total = parts[0]
            for b in range(1, n):
                total = total + parts[b]
            mean = jnp.sum(total, axis=-1, keepdims=True) / d
            parts = [p - mean for p in parts]
            square = parts[0] * parts[0]
            for b in range(1, n):
                square = square + parts[b] * parts[b]
            spread = jnp.sum(square, axis=-1, keepdims=True) / d
            scale = lax.rsqrt(spread + norm_epsilon)
            for b in range(n):
                cols = pl.ds(b * nc, nc)
                dest_ref[pl.ds(m, tm), cols] = (
                    parts[b] * scale * gain_ref[:, cols]
                ).astype(BF)
            return 0

        lax.fori_loop(0, rows // tm, unit, 0)

    def square_relu():
        def unit(i, _):
            m = pl.multiple_of((i % (both // 128)) * 128, 128)
            c = pl.multiple_of((i // (both // 128)) * tn, tn)
            v = jnp.maximum(acc[pl.ds(m, 128), pl.ds(c, tn)], 0.0)
            hid[pl.ds(m, 128), pl.ds(c, tn)] = (v * v).astype(BF)
            return 0

        lax.fori_loop(0, (both // 128) * (ff // tn), unit, 0)

    mix_sem, first_sem, low_sem = 1, 1 + n, 2 + n
    give = mate_copy(first_sem, fst.at[pl.ds(0, rows)], fst.at[pl.ds(rows, rows)])

    plan = {}

    def after(ti, h, which, work):
        plan.setdefault((ti, h, which), []).append(work)

    def project_at(h):
        def work():
            if h:
                arrived(0, h)
            project(h)

        return work

    def mixout_at(h):
        def work():
            if h:
                arrived(1, h)
            lower(mixed, wb, h, precv1, mix_sem)

        return work

    def raise_at(h):
        def work():
            if h:
                arrived(2, h)
            raise_(h)

        return work

    def lower_at(h):
        def work():
            if h:
                arrived(3, h)
            lower(hid, wd, h, precv2, low_sem)

        return work

    def first_half():
        for c in mate_blocks(mix_sem, precv1):
            c.wait_recv()
        norm(tok, precv1, norm1_ref, fst)
        give.start()

    def start_raise():
        give.wait_recv()
        raise_(0)

    after(0, 1, 0, lambda: project(0))
    for h in range(1, half - 1):
        after(0, h + 1, 1, project_at(h))
    after(1, 1, 0, project_at(half - 1))
    after(1, 1, 1, project_at(half))
    after(1, 2, 0, mix)
    after(1, half - 1, 0, mixout_at(0))
    for h in range(1, half - 1):
        after(1, half - 1 if h < half - 2 else half, 0, mixout_at(h))
    after(2, 1, 0, mixout_at(half - 1))
    after(2, 1, 0, mixout_at(half))
    after(2, 1, 1, first_half)
    after(2, 2, 0, start_raise)
    for h in range(1, half - 1):
        after(2, h + 1, 1, raise_at(h))
    after(3, 1, 0, raise_at(half - 1))
    after(3, 1, 1, raise_at(half))
    after(3, 1, 1, square_relu)

    def start_lower():
        for c in mate_blocks(mix_sem, precv1):
            c.wait_send()
        lower_at(0)()

    after(3, 2, 0, start_lower)
    for h in range(1, half - 1):
        after(3, h + 1, 1, lower_at(h))
    after(3, half, 0, lower_at(half - 1))
    after(3, half, 0, lower_at(half))

    for ti in range(4):
        for e in events(ti):
            event(*e)
            for work in plan.get(e, ()):
                work()

    for c in mate_blocks(low_sem, precv2):
        c.wait_recv()
    norm(fst, precv2, norm2_ref, out_ref)

    for c in mate_blocks(low_sem, precv2):
        c.wait_send()
    give.wait_send()
    share.wait_send()
    for key in copies:
        copies[key].wait_send()


def fits(mesh, args):
    n = mesh.shape["fs"]
    tokens, outer_weight = args[0], args[1]
    d, wch = outer_weight.shape[0] * n, outer_weight.shape[1]
    ff = args[7].shape[1]
    rows = tokens.shape[0]
    return (
        mesh.shape["rep"] == 2
        and mesh.shape["tp"] == 2
        and n % 2 == 0
        and n >= 8
        and (d // n) % 128 == 0
        and wch % 256 == 0
        and ff % 256 == 0
        and rows % SEQ == 0
    )


def fused(mesh, *args):
    (
        tokens,
        outer_weight,
        inner_weight,
        value_weight,
        conv_taps,
        mix_out,
        norm_first,
        up_weight,
        down_weight,
        norm_second,
    ) = args
    n = mesh.shape["fs"]
    rows, d = tokens.shape
    ks, wch = outer_weight.shape
    ff = up_weight.shape[1]
    nc = mix_out.shape[1]
    both = 2 * rows
    anywhere = pl.BlockSpec(memory_space=pl.ANY)
    vmem = pl.BlockSpec(memory_space=pltpu.VMEM)
    messages = 4 * (3 * n - 3)
    pairs = 2 + 2 * n
    return pl.pallas_call(
        functools.partial(layer_kernel, n),
        out_shape=jax.ShapeDtypeStruct((rows, d), BF),
        in_specs=[
            anywhere,
            anywhere,
            anywhere,
            anywhere,
            vmem,
            anywhere,
            vmem,
            anywhere,
            anywhere,
            vmem,
        ],
        out_specs=vmem,
        scratch_shapes=[
            pltpu.VMEM((3, n, ks, wch), BF),
            pltpu.VMEM((n, wch, nc), BF),
            pltpu.VMEM((n, ks, ff), BF),
            pltpu.VMEM((n, ff, nc), BF),
            pltpu.VMEM((3, ks, wch), F32),
            pltpu.VMEM((wch, nc), F32),
            pltpu.VMEM((ff, nc), F32),
            pltpu.VMEM((both, d), BF),
            pltpu.VMEM((both, max(3 * wch, ff)), F32),
            pltpu.VMEM((both, wch), BF),
            pltpu.VMEM((n, rows, nc), F32),
            pltpu.VMEM((n, rows, nc), BF),
            pltpu.VMEM((n, rows, nc), BF),
            pltpu.VMEM((n, rows, nc), BF),
            pltpu.VMEM((both, d), BF),
            pltpu.VMEM((both, ff), BF),
            pltpu.SemaphoreType.DMA((7,)),
            pltpu.SemaphoreType.DMA((messages,)),
            pltpu.SemaphoreType.DMA((messages,)),
            pltpu.SemaphoreType.DMA((pairs,)),
            pltpu.SemaphoreType.DMA((pairs,)),
        ],
        compiler_params=pltpu.CompilerParams(
            collective_id=0, has_side_effects=True, vmem_limit_bytes=67043328
        ),
        name="layer",
    )(
        tokens,
        outer_weight,
        inner_weight,
        value_weight,
        conv_taps,
        mix_out,
        norm_first.reshape(1, d),
        up_weight,
        down_weight,
        norm_second.reshape(1, d),
    )


def solution(mesh):
    def body(*args):
        return fused(mesh, *args) if fits(mesh, args) else local(*args)

    return jax.shard_map(
        body,
        mesh=mesh,
        in_specs=(
            P(("rep", "fs", "tp"), None),
            P("fs", "tp"),
            P("fs", "tp"),
            P("fs", "tp"),
            P(None, "tp"),
            P("tp", "fs"),
            P(),
            P("fs", "tp"),
            P("tp", "fs"),
            P(),
        ),
        out_specs=P(("rep", "fs", "tp"), None),
        check_vma=False,
    )
```

```python
import functools

import jax
import jax.numpy as jnp
from jax import lax
from jax.experimental import pallas as pl
from jax.experimental.pallas import tpu as pltpu
from jax.sharding import PartitionSpec as P

SEQ = 128


residual_scale = 2.0**0.25
norm_epsilon = 1e-05


def layer_norm(values, scaling):
    center = values - jnp.mean(values, axis=-1, keepdims=True)
    spread = jnp.mean(center * center, axis=-1, keepdims=True)
    return center * lax.rsqrt(spread + norm_epsilon) * scaling


def short_conv(product, conv_taps):
    places = jnp.arange(product.shape[0], dtype=jnp.int32) % SEQ
    blank = jnp.zeros((1, product.shape[1]), jnp.float32)
    before = jnp.concatenate([blank, product[:-1]], axis=0)
    after = jnp.concatenate([product[1:], blank], axis=0)
    before = jnp.where((places > 0)[:, None], before, 0.0)
    after = jnp.where((places < SEQ - 1)[:, None], after, 0.0)
    return conv_taps[0] * before + conv_taps[1] * product + conv_taps[2] * after


def local(
    tokens,
    outer_weight,
    inner_weight,
    value_weight,
    conv_taps,
    mix_out,
    norm_first,
    up_weight,
    down_weight,
    norm_second,
):
    grouped = lax.all_gather(tokens, "tp", axis=0, tiled=True)
    outer_bf = outer_weight.astype(jnp.bfloat16)
    inner_bf = inner_weight.astype(jnp.bfloat16)
    value_bf = value_weight.astype(jnp.bfloat16)
    outer_full, inner_full, value_full = (
        lax.all_gather(outer_bf, "fs", axis=0, tiled=True),
        lax.all_gather(inner_bf, "fs", axis=0, tiled=True),
        lax.all_gather(value_bf, "fs", axis=0, tiled=True),
    )
    outer = jnp.dot(grouped, outer_full, preferred_element_type=jnp.float32)
    inner = jnp.dot(grouped, inner_full, preferred_element_type=jnp.float32)
    value = jnp.dot(grouped, value_full, preferred_element_type=jnp.float32)
    mixed = (outer * short_conv(inner * value, conv_taps)).astype(jnp.bfloat16)
    mixout_full = lax.all_gather(mix_out.astype(jnp.bfloat16), "fs", axis=1, tiled=True)
    selected = mixed
    mixing = lax.psum_scatter(
        jnp.dot(selected, mixout_full, preferred_element_type=jnp.float32).astype(jnp.bfloat16),
        "tp",
        scatter_dimension=0,
        tiled=True,
    ).astype(jnp.float32)
    first = layer_norm(residual_scale * tokens.astype(jnp.float32) + mixing, norm_first).astype(
        jnp.bfloat16
    )
    grouped_first = lax.all_gather(first, "tp", axis=0, tiled=True)
    upward_bf = up_weight.astype(jnp.bfloat16)
    upward_full = lax.all_gather(upward_bf, "fs", axis=0, tiled=True)
    raised = jnp.dot(grouped_first, upward_full, preferred_element_type=jnp.float32)
    raised = jax.nn.relu(raised)
    hidden = (raised * raised).astype(jnp.bfloat16)
    down_full = lax.all_gather(down_weight.astype(jnp.bfloat16), "fs", axis=1, tiled=True)
    selected = hidden
    lowered = lax.psum_scatter(
        jnp.dot(selected, down_full, preferred_element_type=jnp.float32).astype(jnp.bfloat16),
        "tp",
        scatter_dimension=0,
        tiled=True,
    ).astype(jnp.float32)
    return layer_norm(residual_scale * first.astype(jnp.float32) + lowered, norm_second).astype(
        jnp.bfloat16
    )


MESH = pl.DeviceIdType.MESH
BF = jnp.bfloat16
F32 = jnp.float32


def dot(a, b):
    return jnp.dot(a, b, preferred_element_type=F32)


def third_rows(rows):
    return (rows // 3 + 8) // 16 * 16


def layer_kernel(
    n,
    tokens_hbm,
    outer_hbm,
    inner_hbm,
    value_hbm,
    taps_ref,
    mix_hbm,
    norm1_ref,
    up_hbm,
    down_hbm,
    norm2_ref,
    out_ref,
    wa,
    wb,
    wc,
    wd,
    tok,
    acc,
    mixed,
    own,
    psend,
    precv1,
    precv2,
    xsend,
    xrecv,
    fst,
    hid,
    load_sem,
    ring_send,
    ring_recv,
    tp_send,
    tp_recv,
    x_send,
    x_recv,
):
    half = n // 2
    r = lax.axis_index("rep")
    f = lax.axis_index("fs")
    t = lax.axis_index("tp")
    rows = tokens_hbm.shape[0]
    both = 2 * rows
    d = tokens_hbm.shape[1]
    ks = wa.shape[2]
    wch = wa.shape[3]
    ff = wc.shape[1]
    nc = wb.shape[2]

    odd = f % 2
    pos = (1 - odd) * (f // 2) + odd * (n - 1 - f // 2)

    def at(place):
        p = (place + 2 * n) % n
        hi = p // half
        return (1 - hi) * (2 * p) + hi * (2 * (n - 1 - p) + 1)

    right = {"fs": at(pos + 1)}
    left = {"fs": at(pos - 1)}
    across = {"rep": 1 - r}
    mate = {"tp": 1 - t}

    mine = pl.multiple_of(r * ff, 128)
    first_down = min(ff, both)
    rest_down = ff - first_down
    loads = [
        pltpu.make_async_copy(
            src, acc.at[pl.ds(i * ks, ks), pl.ds(0, wch)], load_sem.at[i]
        )
        for i, src in enumerate((outer_hbm, inner_hbm, value_hbm))
    ]
    loads += [
        pltpu.make_async_copy(mix_hbm, own.at[0, pl.ds(0, wch)], load_sem.at[3]),
        pltpu.make_async_copy(
            up_hbm.at[:, pl.ds(mine, ff)],
            acc.at[pl.ds(3 * ks, ks), pl.ds(0, ff)],
            load_sem.at[4],
        ),
        pltpu.make_async_copy(
            down_hbm.at[pl.ds(mine, first_down)],
            own.at[1, pl.ds(0, first_down)],
            load_sem.at[5],
        ),
        pltpu.make_async_copy(tokens_hbm, tok.at[pl.ds(0, rows)], load_sem.at[6]),
    ]
    if rest_down:
        loads.append(
            pltpu.make_async_copy(
                down_hbm.at[pl.ds(mine + first_down, rest_down)],
                own.at[2, pl.ds(0, rest_down)],
                load_sem.at[7],
            )
        )
    for load in loads:
        load.start()

    barrier = pltpu.get_barrier_semaphore()
    for device in (right, left, across, mate):
        pl.semaphore_signal(barrier, inc=1, device_id=device, device_id_type=MESH)
    pl.semaphore_wait(barrier, 4)

    def mate_copy(i, src, dst):
        return pltpu.make_async_remote_copy(
            src_ref=src,
            dst_ref=dst,
            send_sem=tp_send.at[i],
            recv_sem=tp_recv.at[i],
            device_id=mate,
            device_id_type=MESH,
        )

    def across_copy(i, src, dst):
        return pltpu.make_async_remote_copy(
            src_ref=src,
            dst_ref=dst,
            send_sem=x_send.at[i],
            recv_sem=x_recv.at[i],
            device_id=across,
            device_id_type=MESH,
        )

    def piece(ti, which, owner):
        if ti == 0:
            return wa.at[2 if which else r, owner]
        if ti == 1:
            u = third_rows(wch)
            if which:
                return wb.at[owner, pl.ds(2 * u, wch - 2 * u)]
            return wb.at[owner, pl.ds(pl.multiple_of(r * u, 16), u)]
        if ti == 2:
            u = ks // 2
            return wc.at[pl.ds(pl.multiple_of(owner * ks + which * u, 16), u)]
        return wd.at[owner, pl.ds(which * (ff // 2), ff // 2)]

    per = 6 * half - 3
    index = {}
    for h in range(1, half + 1):
        for kind in ("Rq", "Rp", "Lq", "Lp", "XR", "XL"):
            if h == half and kind in ("Rp", "Lq", "XL"):
                continue
            index[kind, h] = len(index)

    copies = {}

    def message(ti, kind, h):
        key = (ti, kind, h)
        if key not in copies:
            which = int(kind[1] == "p")
            if kind[0] == "R":
                src, device = at(pos - (h - 1)), right
            elif kind[0] == "L":
                src, device = at(pos + (h - 1)), left
            else:
                src, device = at(pos - h if kind == "XR" else pos + h), across
            i = ti * per + index[kind, h]
            ref = piece(ti, which, src)
            copies[key] = pltpu.make_async_remote_copy(
                src_ref=ref,
                dst_ref=ref,
                send_sem=ring_send.at[i],
                recv_sem=ring_recv.at[i],
                device_id=device,
                device_id_type=MESH,
            )
        return copies[key]

    def send(ti, kind, h):
        if ti < 4 and (kind, h) in index and (ti < 2 or kind[0] != "X"):
            message(ti, kind, h).start()

    def got(ti, kind, h):
        message(ti, kind, h).wait_recv()

    def event(ti, h, which):
        if which == 0:
            got(ti, "Rq", h)
            send(ti, "Rq", h + 1)
            send(ti, "XR", h)
            if h < half:
                got(ti, "Lq", h)
                if h + 1 < half:
                    send(ti, "Lq", h + 1)
                else:
                    send(ti + 1, "Lq", 1)
                send(ti, "XL", h)
            else:
                send(ti + 1, "Rp", 1)
                got(ti, "Lp", h)
                send(ti + 1, "Lp", 1)
        else:
            got(ti, "Rp", h)
            if h + 1 < half:
                send(ti, "Rp", h + 1)
            else:
                send(ti + 1, "Rq", 1)
            got(ti, "Lp", h)
            send(ti, "Lp", h + 1)

    def events(ti):
        out = []
        for h in range(1, half + 1):
            out.append((ti, h, 0))
            if h < half:
                out.append((ti, h, 1))
        return out

    def arrived(ti, h):
        got(ti, "XR", h)
        if h < half:
            got(ti, "XL", h)

    def owners(h):
        if h == 0:
            return [f]
        if h == half:
            return [at(pos + half)]
        return [at(pos - h), at(pos + h)]

    for i in range(3):
        loads[i].wait()
        wa[i, f] = acc[pl.ds(i * ks, ks), pl.ds(0, wch)].astype(BF)
    send(0, "Rq", 1)
    send(0, "Lq", 1)
    send(0, "Rp", 1)
    send(0, "Lp", 1)
    share = mate_copy(0, tokens_hbm, tok.at[pl.ds(rows, rows)])
    share.start()
    loads[3].wait()
    wb[f] = own[0, pl.ds(0, wch)].astype(BF)
    loads[4].wait()
    wc[pl.ds(pl.multiple_of(f * ks, 16), ks), :] = acc[
        pl.ds(3 * ks, ks), pl.ds(0, ff)
    ].astype(BF)
    loads[5].wait()
    wd[f, pl.ds(0, first_down)] = own[1, pl.ds(0, first_down)].astype(BF)
    if rest_down:
        loads[7].wait()
        wd[f, pl.ds(first_down, rest_down)] = own[2, pl.ds(0, rest_down)].astype(BF)
    loads[6].wait()
    share.wait_recv()

    tn = 256
    pieces = 2
    pr = rows // pieces
    mix_sem, first_sem = 1, 1 + n
    diag_sem = first_sem + pieces
    far_sem = diag_sem + pieces
    near_sem = far_sem + n
    OWN, TWIN, MATE, DIAG = 0, rows, 2 * rows, 3 * rows

    def accumulate(x_ref, gap, h, weight, width, dest):
        who = owners(h)

        def unit(i, _):
            side = i % 2
            c = i // 2
            total = None
            for o in who:
                x = x_ref[
                    pl.ds(pl.multiple_of(side * gap, 16), rows),
                    pl.ds(pl.multiple_of(o * ks, 128), ks),
                ]
                term = dot(x, weight(o, pl.ds(pl.multiple_of(c * tn, tn), tn)))
                total = term if total is None else total + term
            view = dest(pl.multiple_of(side * rows, 16), c)
            if h == 0:
                view[...] = total
            else:
                view[...] += total
            return 0

        lax.fori_loop(0, 2 * (width // tn), unit, 0)

    def acc_at(base):
        def dest(m, c):
            return acc.at[
                pl.ds(base + m, rows), pl.ds(pl.multiple_of(c * tn, tn), tn)
            ]

        return dest

    def project(h):
        for i in range(3):
            dest = (
                acc_at(i * both)
                if i < 2
                else lambda m, c: own.at[c, pl.ds(m, rows), :]
            )
            accumulate(tok, rows, h, lambda o, c, i=i: wa[i, o, :, c], wch, dest)

    def raise_near(h):
        def weight(o, c):
            return wc[pl.ds(pl.multiple_of(o * ks, 16), ks), c]

        accumulate(fst, MATE, h, weight, ff, acc_at(0))

    def raise_far(start):
        def unit(i, _):
            c = pl.ds(pl.multiple_of(i * tn, tn), tn)
            v = jnp.maximum(dot(fst[pl.ds(start, pr), :], wc[:, c]), 0.0)
            hid[pl.ds(start, pr), c] = (v * v).astype(BF)
            return 0

        lax.fori_loop(0, ff // tn, unit, 0)

    def numbered(h):
        return [(0 if h == 0 else 2 * h - 1 + k, o) for k, o in enumerate(owners(h))]

    every = [item for h in range(half + 1) for item in numbered(h)]

    def mix_block(k, o):
        return mate_copy(mix_sem + k, psend.at[o, pl.ds(0, rows)], precv1.at[o])

    def near_block(k, o):
        part = pl.ds(0, rows)
        return mate_copy(near_sem + k, psend.at[o, part], precv2.at[o, part])

    def far_block(k, o):
        part = pl.ds(rows, rows)
        return mate_copy(far_sem + k, psend.at[o, part], precv2.at[o, part])

    def across_block(k, o):
        return across_copy(pieces + k, xsend.at[o], xrecv.at[o])

    def mixout(h):
        for k, o in numbered(h):
            psend[o, pl.ds(0, rows)] = dot(mixed[pl.ds(rows, rows), :], wb[o]).astype(BF)
            mix_block(k, o).start()
            own[o, pl.ds(0, rows)] = dot(mixed[pl.ds(0, rows), :], wb[o])

    def lower_far(h):
        for k, o in numbered(h):
            psend[o, pl.ds(rows, rows)] = dot(hid[pl.ds(DIAG, rows), :], wd[o]).astype(BF)
            far_block(k, o).start()
            own[o, pl.ds(rows, rows)] = dot(hid[pl.ds(TWIN, rows), :], wd[o])

    def pass_across(h):
        for k, o in numbered(h):
            far_block(k, o).wait_recv()
            part = pl.ds(rows, rows)
            xsend[o] = (own[o, part] + precv2[o, part].astype(F32)).astype(BF)
            across_block(k, o).start()

    def lower_near(h):
        for k, o in numbered(h):
            psend[o, pl.ds(0, rows)] = dot(hid[pl.ds(MATE, rows), :], wd[o]).astype(BF)
            near_block(k, o).start()
            own[o, pl.ds(0, rows)] = dot(hid[pl.ds(OWN, rows), :], wd[o])

    def mix():
        seq = SEQ

        def unit(i, _):
            m = pl.multiple_of((i % (both // seq)) * seq, seq)
            c = pl.multiple_of((i // (both // seq)) * tn, tn)
            o = acc[pl.ds(m, seq), pl.ds(c, tn)]
            p = (
                acc[pl.ds(both + m, seq), pl.ds(c, tn)]
                * own[i // (both // seq), pl.ds(m, seq), :]
            )
            place = lax.broadcasted_iota(jnp.int32, p.shape, 0)
            before = jnp.where(place > 0, pltpu.roll(p, 1, 0), 0.0)
            after = jnp.where(place < seq - 1, pltpu.roll(p, seq - 1, 0), 0.0)
            taps = taps_ref[:, pl.ds(c, tn)]
            conv = taps[0:1] * before + taps[1:2] * p + taps[2:3] * after
            mixed[pl.ds(m, seq), pl.ds(c, tn)] = (o * conv).astype(BF)
            return 0

        lax.fori_loop(0, (both // seq) * (wch // tn), unit, 0)

    def norm(base_ref, terms, gain_ref, dest_ref, start, count):
        tm = 32

        def unit(i, _):
            m = pl.multiple_of(start + i * tm, tm)
            parts = []
            for b in range(n):
                part = (
                    residual_scale
                    * base_ref[pl.ds(m, tm), pl.ds(b * nc, nc)].astype(F32)
                    + own[b, pl.ds(m, tm)]
                )
                for term in terms:
                    part = part + term[b, pl.ds(m, tm)].astype(F32)
                parts.append(part)
            total = parts[0]
            for b in range(1, n):
                total = total + parts[b]
            mean = jnp.sum(total, axis=-1, keepdims=True) / d
            parts = [p - mean for p in parts]
            square = parts[0] * parts[0]
            for b in range(1, n):
                square = square + parts[b] * parts[b]
            spread = jnp.sum(square, axis=-1, keepdims=True) / d
            scale = lax.rsqrt(spread + norm_epsilon)
            for b in range(n):
                cols = pl.ds(b * nc, nc)
                dest_ref[pl.ds(m, tm), cols] = (
                    parts[b] * scale * gain_ref[:, cols]
                ).astype(BF)
            return 0

        lax.fori_loop(0, count // tm, unit, 0)

    def square_near():
        def unit(i, _):
            tiles = rows // 128
            side = i % 2
            m = pl.multiple_of(((i // 2) % tiles) * 128, 128)
            c = pl.ds(pl.multiple_of((i // (2 * tiles)) * tn, tn), tn)
            v = jnp.maximum(acc[pl.ds(side * rows + m, 128), c], 0.0)
            hid[pl.ds(side * MATE + m, 128), c] = (v * v).astype(BF)
            return 0

        lax.fori_loop(0, 2 * (rows // 128) * (ff // tn), unit, 0)

    def near_first(p):
        return mate_copy(
            first_sem + p, fst.at[pl.ds(p * pr, pr)], fst.at[pl.ds(MATE + p * pr, pr)]
        )

    def twin_first(p):
        return across_copy(
            p, fst.at[pl.ds(p * pr, pr)], fst.at[pl.ds(TWIN + p * pr, pr)]
        )

    def diag_first(p):
        return mate_copy(
            diag_sem + p,
            fst.at[pl.ds(TWIN + p * pr, pr)],
            fst.at[pl.ds(DIAG + p * pr, pr)],
        )

    def make_first():
        for k, o in every:
            mix_block(k, o).wait_recv()
        for p in range(pieces):
            norm(tok, (precv1,), norm1_ref, fst, p * pr, pr)
            twin_first(p).start()
            near_first(p).start()

    def take_near():
        for p in range(pieces):
            near_first(p).wait_recv()

    def relay_first(p):
        twin_first(p).wait_recv()
        diag_first(p).start()

    def far(p):
        raise_far(TWIN + p * pr)
        diag_first(p).wait_recv()
        raise_far(DIAG + p * pr)

    def free_sends():
        for k, o in every:
            mix_block(k, o).wait_send()

    plan = {}

    def after(ti, h, which, *work):
        plan.setdefault((ti, h, which), []).extend(work)

    def project_at(h):
        def work():
            if h:
                arrived(0, h)
            project(h)

        return work

    def mixout_at(h):
        def work():
            if h:
                arrived(1, h)
            mixout(h)

        return work

    def do(function, *values):
        return lambda: function(*values)

    last = half - 1
    after(0, 1, 0, project_at(0))
    for h in range(1, last):
        after(0, h + 1, 1, project_at(h))
    after(1, 1, 0, project_at(last))
    after(1, 1, 1, project_at(half))
    after(1, 2, 0, mix)
    after(1, last, 0, mixout_at(0))
    for h in range(1, half + 1):
        after(1, last if h < last - 1 else half, 0, mixout_at(h))
    after(1, half, 0, make_first)
    after(2, 1, 0, take_near, do(raise_near, 0))
    for h in range(1, last):
        after(2, h + 1, 1, do(raise_near, h))
    after(2, last, 0, do(relay_first, 0))
    after(2, half, 0, do(raise_near, last), do(raise_near, half), do(far, 0))
    for p in range(1, pieces):
        after(3, 1, 0, do(relay_first, p), do(far, p))
    after(3, 1, 1, free_sends, do(lower_far, 0), do(lower_far, 1))
    after(3, 1, 1, do(pass_across, 0))
    after(3, 2, 0, do(pass_across, 1), square_near)
    for h in range(2, half):
        after(3, h, 1, do(lower_far, h), do(lower_near, h - 2), do(pass_across, h))
    after(3, half, 0, do(lower_far, half), do(lower_near, half - 2))
    after(3, half, 0, do(pass_across, half))
    after(3, half, 0, do(lower_near, half - 1), do(lower_near, half))

    for ti in range(4):
        for e in events(ti):
            event(*e)
            for work in plan.get(e, ()):
                work()

    for k, o in every:
        near_block(k, o).wait_recv()
    for k, o in every:
        across_block(k, o).wait_recv()
    norm(fst, (precv2, xrecv), norm2_ref, out_ref, 0, rows)

    for k, o in every:
        near_block(k, o).wait_send()
        far_block(k, o).wait_send()
        across_block(k, o).wait_send()
    for p in range(pieces):
        near_first(p).wait_send()
        twin_first(p).wait_send()
        diag_first(p).wait_send()
    share.wait_send()
    for key in copies:
        copies[key].wait_send()


def fits(mesh, args):
    n = mesh.shape["fs"]
    rows, d = args[0].shape
    ks, wch = args[1].shape
    nc = args[5].shape[1]
    ff = args[7].shape[1] // 2
    return (
        mesh.shape["rep"] == 2
        and mesh.shape["tp"] == 2
        and n % 2 == 0
        and n >= 8
        and ks % 128 == 0
        and nc == 256
        and wch % 256 == 0
        and ff % 256 == 0
        and wch // 256 <= n
        and wch <= 2 * rows
        and ff <= 4 * rows
        and ks <= rows
        and rows % SEQ == 0
    )


def fused(mesh, *args):
    (
        tokens,
        outer_weight,
        inner_weight,
        value_weight,
        conv_taps,
        mix_out,
        norm_first,
        up_weight,
        down_weight,
        norm_second,
    ) = args
    n = mesh.shape["fs"]
    rows, d = tokens.shape
    ks, wch = outer_weight.shape
    ff = up_weight.shape[1] // 2
    nc = mix_out.shape[1]
    both = 2 * rows
    anywhere = pl.BlockSpec(memory_space=pl.ANY)
    vmem = pl.BlockSpec(memory_space=pltpu.VMEM)
    messages = 4 * (3 * n - 3)
    pairs = 5 + 3 * n
    return pl.pallas_call(
        functools.partial(layer_kernel, n),
        out_shape=jax.ShapeDtypeStruct((rows, d), BF),
        in_specs=[
            anywhere,
            anywhere,
            anywhere,
            anywhere,
            vmem,
            anywhere,
            vmem,
            anywhere,
            anywhere,
            vmem,
        ],
        out_specs=vmem,
        scratch_shapes=[
            pltpu.VMEM((3, n, ks, wch), BF),
            pltpu.VMEM((n, wch, nc), BF),
            pltpu.VMEM((n * ks, ff), BF),
            pltpu.VMEM((n, ff, nc), BF),
            pltpu.VMEM((both, d), BF),
            pltpu.VMEM((2 * both, max(wch, ff)), F32),
            pltpu.VMEM((both, wch), BF),
            pltpu.VMEM((n, both, nc), F32),
            pltpu.VMEM((n, both, nc), BF),
            pltpu.VMEM((n, rows, nc), BF),
            pltpu.VMEM((n, both, nc), BF),
            pltpu.VMEM((n, rows, nc), BF),
            pltpu.VMEM((n, rows, nc), BF),
            pltpu.VMEM((2 * both, d), BF),
            pltpu.VMEM((2 * both, ff), BF),
            pltpu.SemaphoreType.DMA((8,)),
            pltpu.SemaphoreType.DMA((messages,)),
            pltpu.SemaphoreType.DMA((messages,)),
            pltpu.SemaphoreType.DMA((pairs,)),
            pltpu.SemaphoreType.DMA((pairs,)),
            pltpu.SemaphoreType.DMA((2 + n,)),
            pltpu.SemaphoreType.DMA((2 + n,)),
        ],
        compiler_params=pltpu.CompilerParams(
            collective_id=0, has_side_effects=True, vmem_limit_bytes=67043328
        ),
        name="layer",
    )(
        tokens,
        outer_weight,
        inner_weight,
        value_weight,
        conv_taps,
        mix_out,
        norm_first.reshape(1, d),
        up_weight,
        down_weight,
        norm_second.reshape(1, d),
    )


def solution(mesh):
    def body(*args):
        return fused(mesh, *args) if fits(mesh, args) else local(*args)

    return jax.shard_map(
        body,
        mesh=mesh,
        in_specs=(
            P(("rep", "fs", "tp"), None),
            P("fs", "tp"),
            P("fs", "tp"),
            P("fs", "tp"),
            P(None, "tp"),
            P("tp", "fs"),
            P(),
            P("fs", "tp"),
            P("tp", "fs"),
            P(),
        ),
        out_specs=P(("rep", "fs", "tp"), None),
        check_vma=False,
    )
```

```python
import functools

import jax
import jax.numpy as jnp
from jax import lax
from jax.experimental import pallas as pl
from jax.experimental.pallas import tpu as pltpu
from jax.sharding import PartitionSpec as P

SEQ = 128


residual_scale = 2.0**0.25
norm_epsilon = 1e-05


def layer_norm(values, scaling):
    center = values - jnp.mean(values, axis=-1, keepdims=True)
    spread = jnp.mean(center * center, axis=-1, keepdims=True)
    return center * lax.rsqrt(spread + norm_epsilon) * scaling


def short_conv(product, conv_taps):
    places = jnp.arange(product.shape[0], dtype=jnp.int32) % SEQ
    blank = jnp.zeros((1, product.shape[1]), jnp.float32)
    before = jnp.concatenate([blank, product[:-1]], axis=0)
    after = jnp.concatenate([product[1:], blank], axis=0)
    before = jnp.where((places > 0)[:, None], before, 0.0)
    after = jnp.where((places < SEQ - 1)[:, None], after, 0.0)
    return conv_taps[0] * before + conv_taps[1] * product + conv_taps[2] * after


def local(
    tokens,
    outer_weight,
    inner_weight,
    value_weight,
    conv_taps,
    mix_out,
    norm_first,
    up_weight,
    down_weight,
    norm_second,
):
    grouped = lax.all_gather(tokens, "tp", axis=0, tiled=True)
    outer_bf = outer_weight.astype(jnp.bfloat16)
    inner_bf = inner_weight.astype(jnp.bfloat16)
    value_bf = value_weight.astype(jnp.bfloat16)
    outer_full, inner_full, value_full = (
        lax.all_gather(outer_bf, "fs", axis=0, tiled=True),
        lax.all_gather(inner_bf, "fs", axis=0, tiled=True),
        lax.all_gather(value_bf, "fs", axis=0, tiled=True),
    )
    outer = jnp.dot(grouped, outer_full, preferred_element_type=jnp.float32)
    inner = jnp.dot(grouped, inner_full, preferred_element_type=jnp.float32)
    value = jnp.dot(grouped, value_full, preferred_element_type=jnp.float32)
    mixed = (outer * short_conv(inner * value, conv_taps)).astype(jnp.bfloat16)
    mixout_full = lax.all_gather(mix_out.astype(jnp.bfloat16), "fs", axis=1, tiled=True)
    selected = mixed
    mixing = lax.psum_scatter(
        jnp.dot(selected, mixout_full, preferred_element_type=jnp.float32).astype(jnp.bfloat16),
        "tp",
        scatter_dimension=0,
        tiled=True,
    ).astype(jnp.float32)
    first = layer_norm(residual_scale * tokens.astype(jnp.float32) + mixing, norm_first).astype(
        jnp.bfloat16
    )
    grouped_first = lax.all_gather(first, "tp", axis=0, tiled=True)
    upward_bf = up_weight.astype(jnp.bfloat16)
    upward_full = lax.all_gather(upward_bf, "fs", axis=0, tiled=True)
    raised = jnp.dot(grouped_first, upward_full, preferred_element_type=jnp.float32)
    raised = jax.nn.relu(raised)
    hidden = (raised * raised).astype(jnp.bfloat16)
    down_full = lax.all_gather(down_weight.astype(jnp.bfloat16), "fs", axis=1, tiled=True)
    selected = hidden
    lowered = lax.psum_scatter(
        jnp.dot(selected, down_full, preferred_element_type=jnp.float32).astype(jnp.bfloat16),
        "tp",
        scatter_dimension=0,
        tiled=True,
    ).astype(jnp.float32)
    return layer_norm(residual_scale * first.astype(jnp.float32) + lowered, norm_second).astype(
        jnp.bfloat16
    )


MESH = pl.DeviceIdType.MESH
BF = jnp.bfloat16
F32 = jnp.float32


def dot(a, b):
    return jnp.dot(a, b, preferred_element_type=F32)


def layer_kernel(
    n,
    tokens_hbm,
    outer_hbm,
    inner_hbm,
    value_hbm,
    taps_ref,
    mix_hbm,
    norm1_ref,
    up_hbm,
    down_hbm,
    norm2_ref,
    out_ref,
    wa,
    wb,
    wc,
    wd,
    tok,
    acc,
    mixed,
    own,
    psend,
    precv1,
    precv2,
    xsend,
    xrecv,
    fst,
    hid,
    load_sem,
    ring_send,
    ring_recv,
    tp_send,
    tp_recv,
    x_send,
    x_recv,
):
    half = n // 2
    r = lax.axis_index("rep")
    f = lax.axis_index("fs")
    t = lax.axis_index("tp")
    rows = tokens_hbm.shape[0]
    both = 2 * rows
    d = tokens_hbm.shape[1]
    ks = wa.shape[2]
    wch = wa.shape[3]
    ff = wc.shape[1]
    nc = wb.shape[2]

    odd = f % 2
    pos = (1 - odd) * (f // 2) + odd * (n - 1 - f // 2)

    def at(place):
        p = (place + 2 * n) % n
        hi = p // half
        return (1 - hi) * (2 * p) + hi * (2 * (n - 1 - p) + 1)

    right = {"fs": at(pos + 1)}
    left = {"fs": at(pos - 1)}
    across = {"rep": 1 - r}
    mate = {"tp": 1 - t}

    mine = pl.multiple_of(r * ff, 128)
    first_down = min(ff, both)
    rest_down = ff - first_down
    loads = [
        pltpu.make_async_copy(
            src, acc.at[pl.ds(i * ks, ks), pl.ds(0, wch)], load_sem.at[i]
        )
        for i, src in enumerate((outer_hbm, inner_hbm, value_hbm))
    ]
    loads += [
        pltpu.make_async_copy(mix_hbm, own.at[0, pl.ds(0, wch)], load_sem.at[3]),
        pltpu.make_async_copy(
            up_hbm.at[:, pl.ds(mine, ff)],
            acc.at[pl.ds(3 * ks, ks), pl.ds(0, ff)],
            load_sem.at[4],
        ),
        pltpu.make_async_copy(
            down_hbm.at[pl.ds(mine, first_down)],
            own.at[1, pl.ds(0, first_down)],
            load_sem.at[5],
        ),
        pltpu.make_async_copy(tokens_hbm, tok.at[pl.ds(0, rows)], load_sem.at[6]),
    ]
    if rest_down:
        loads.append(
            pltpu.make_async_copy(
                down_hbm.at[pl.ds(mine + first_down, rest_down)],
                own.at[2, pl.ds(0, rest_down)],
                load_sem.at[7],
            )
        )
    for load in loads[:3]:
        load.start()

    barrier = pltpu.get_barrier_semaphore()
    for device in (right, left, across, mate):
        pl.semaphore_signal(barrier, inc=1, device_id=device, device_id_type=MESH)
    pl.semaphore_wait(barrier, 4)

    def mate_copy(i, src, dst):
        return pltpu.make_async_remote_copy(
            src_ref=src,
            dst_ref=dst,
            send_sem=tp_send.at[i],
            recv_sem=tp_recv.at[i],
            device_id=mate,
            device_id_type=MESH,
        )

    def across_copy(i, src, dst):
        return pltpu.make_async_remote_copy(
            src_ref=src,
            dst_ref=dst,
            send_sem=x_send.at[i],
            recv_sem=x_recv.at[i],
            device_id=across,
            device_id_type=MESH,
        )

    def piece(ti, which, owner):
        if ti == 0:
            return wa.at[2 if which else r, owner]
        if ti == 1:
            u = wch // 64 * 16
            if which:
                return wb.at[owner, pl.ds(2 * u, wch - 2 * u)]
            return wb.at[owner, pl.ds(pl.multiple_of(r * u, 16), u)]
        if ti == 2:
            u = ks // 2
            return wc.at[pl.ds(pl.multiple_of(owner * ks + which * u, 16), u)]
        return wd.at[owner, pl.ds(which * (ff // 2), ff // 2)]

    per = 6 * half - 3
    index = {}
    for h in range(1, half + 1):
        for kind in ("Rq", "Rp", "Lq", "Lp", "XR", "XL"):
            if h == half and kind in ("Rp", "Lq", "XL"):
                continue
            index[kind, h] = len(index)

    copies = {}

    def message(ti, kind, h):
        key = (ti, kind, h)
        if key not in copies:
            which = int(kind[1] == "p")
            if kind[0] == "R":
                src, device = at(pos - (h - 1)), right
            elif kind[0] == "L":
                src, device = at(pos + (h - 1)), left
            else:
                src, device = at(pos - h if kind == "XR" else pos + h), across
            i = ti * per + index[kind, h]
            ref = piece(ti, which, src)
            copies[key] = pltpu.make_async_remote_copy(
                src_ref=ref,
                dst_ref=ref,
                send_sem=ring_send.at[i],
                recv_sem=ring_recv.at[i],
                device_id=device,
                device_id_type=MESH,
            )
        return copies[key]

    def send(ti, kind, h):
        if ti < 4 and (kind, h) in index and (ti < 2 or kind[0] != "X"):
            message(ti, kind, h).start()

    def got(ti, kind, h):
        message(ti, kind, h).wait_recv()

    def event(ti, h, which):
        if which == 0:
            got(ti, "Rq", h)
            send(ti, "Rq", h + 1)
            send(ti, "XR", h)
            if h == half:
                send(ti + 1, "Rp", 1)
            got(ti, "Lp", h)
            send(ti, "Lp", h + 1)
            if h == half:
                send(ti + 1, "Lq", 1)
        else:
            got(ti, "Rp", h)
            if h + 1 < half:
                send(ti, "Rp", h + 1)
            else:
                send(ti + 1, "Rq", 1)
            got(ti, "Lq", h)
            if h + 1 < half:
                send(ti, "Lq", h + 1)
            else:
                send(ti + 1, "Lp", 1)
            send(ti, "XL", h)

    def events(ti):
        out = []
        for h in range(1, half + 1):
            out.append((ti, h, 0))
            if h < half:
                out.append((ti, h, 1))
        return out

    def arrived(ti, h):
        got(ti, "XR", h)
        if h < half:
            got(ti, "XL", h)

    def owners(h):
        if h == 0:
            return [f]
        if h == half:
            return [at(pos + half)]
        return [at(pos - h), at(pos + h)]

    for i in range(3):
        loads[i].wait()
        wa[i, f] = acc[pl.ds(i * ks, ks), pl.ds(0, wch)].astype(BF)
    send(0, "Rq", 1)
    send(0, "Lp", 1)
    send(0, "Rp", 1)
    send(0, "Lq", 1)
    for load in loads[3:]:
        load.start()
    share = mate_copy(0, tokens_hbm, tok.at[pl.ds(rows, rows)])
    share.start()
    loads[3].wait()
    wb[f] = own[0, pl.ds(0, wch)].astype(BF)
    loads[4].wait()
    wc[pl.ds(pl.multiple_of(f * ks, 16), ks), :] = acc[
        pl.ds(3 * ks, ks), pl.ds(0, ff)
    ].astype(BF)
    loads[5].wait()
    wd[f, pl.ds(0, first_down)] = own[1, pl.ds(0, first_down)].astype(BF)
    if rest_down:
        loads[7].wait()
        wd[f, pl.ds(first_down, rest_down)] = own[2, pl.ds(0, rest_down)].astype(BF)
    loads[6].wait()
    share.wait_recv()

    tn = 256
    pieces = 4
    pr = rows // pieces
    mix_sem, first_sem = 1, 1 + n
    diag_sem = first_sem + pieces
    far_sem = diag_sem + pieces
    near_sem = far_sem + n
    OWN, TWIN, MATE, DIAG = 0, rows, 2 * rows, 3 * rows

    def accumulate(x_ref, gap, h, weight, width, dest):
        who = owners(h)

        def unit(i, _):
            side = i % 2
            c = i // 2
            total = None
            for o in who:
                x = x_ref[
                    pl.ds(pl.multiple_of(side * gap, 16), rows),
                    pl.ds(pl.multiple_of(o * ks, 128), ks),
                ]
                term = dot(x, weight(o, pl.ds(pl.multiple_of(c * tn, tn), tn)))
                total = term if total is None else total + term
            view = dest(pl.multiple_of(side * rows, 16), c)
            if h == 0:
                view[...] = total
            else:
                view[...] += total
            return 0

        lax.fori_loop(0, 2 * (width // tn), unit, 0)

    def acc_at(base):
        def dest(m, c):
            return acc.at[
                pl.ds(base + m, rows), pl.ds(pl.multiple_of(c * tn, tn), tn)
            ]

        return dest

    def project(h, tensors=(0, 1, 2)):
        for i in tensors:
            dest = (
                acc_at(i * both)
                if i < 2
                else lambda m, c: own.at[c, pl.ds(m, rows), :]
            )
            accumulate(tok, rows, h, lambda o, c, i=i: wa[i, o, :, c], wch, dest)

    def raise_part(size, start, x_base, acc_base, hs, new, final):
        who = [o for h in hs for o in owners(h)]
        tiles = ff // tn

        def unit(i, _):
            side = i % 2
            c = pl.ds(pl.multiple_of(i // 2 * tn, tn), tn)
            x_row = pl.multiple_of(x_base + side * MATE + start, 16)
            total = None
            for o in who:
                x = fst[
                    pl.ds(x_row, size), pl.ds(pl.multiple_of(o * ks, 128), ks)
                ]
                term = dot(x, wc[pl.ds(pl.multiple_of(o * ks, 16), ks), c])
                total = term if total is None else total + term
            span = pl.ds(pl.multiple_of(acc_base + side * rows + start, 16), size)
            if not new:
                total = total + acc[span, c]
            if final:
                total = jnp.maximum(total, 0.0)
                hid[pl.ds(x_row, size), c] = (total * total).astype(BF)
            else:
                acc[span, c] = total
            return 0

        lax.fori_loop(0, 2 * tiles, unit, 0)

    def raise_near(h):
        raise_part(rows, 0, OWN, 0, [h], h == 0, h == half)

    def raise_far(p, count, hs):
        raise_part(pr * count, p * pr, TWIN, both, hs, 0 in hs, half in hs)

    def numbered(h):
        return [(0 if h == 0 else 2 * h - 1 + k, o) for k, o in enumerate(owners(h))]

    every = [item for h in range(half + 1) for item in numbered(h)]

    def mix_block(k, o):
        return mate_copy(mix_sem + k, psend.at[o, pl.ds(0, rows)], precv1.at[o])

    def near_block(k, o):
        part = pl.ds(0, rows)
        return mate_copy(near_sem + k, psend.at[o, part], precv2.at[o, part])

    def far_block(k, o):
        part = pl.ds(rows, rows)
        return mate_copy(far_sem + k, psend.at[o, part], precv2.at[o, part])

    def across_block(k, o):
        return across_copy(pieces + k, xsend.at[o], xrecv.at[o])

    def mixout(h):
        for k, o in numbered(h):
            psend[o, pl.ds(0, rows)] = dot(mixed[pl.ds(rows, rows), :], wb[o]).astype(BF)
            mix_block(k, o).start()
            own[o, pl.ds(0, rows)] = dot(mixed[pl.ds(0, rows), :], wb[o])

    def lower_far(h):
        for k, o in numbered(h):
            psend[o, pl.ds(rows, rows)] = dot(hid[pl.ds(DIAG, rows), :], wd[o]).astype(BF)
            far_block(k, o).start()
            own[o, pl.ds(rows, rows)] = dot(hid[pl.ds(TWIN, rows), :], wd[o])

    def pass_across(h):
        for k, o in numbered(h):
            far_block(k, o).wait_recv()
            part = pl.ds(rows, rows)
            xsend[o] = (own[o, part] + precv2[o, part].astype(F32)).astype(BF)
            across_block(k, o).start()

    def lower_near(h):
        for k, o in numbered(h):
            psend[o, pl.ds(0, rows)] = dot(hid[pl.ds(MATE, rows), :], wd[o]).astype(BF)
            near_block(k, o).start()
            own[o, pl.ds(0, rows)] = dot(hid[pl.ds(OWN, rows), :], wd[o])

    def mix():
        seq = SEQ

        def unit(i, _):
            m = pl.multiple_of((i % (both // seq)) * seq, seq)
            c = pl.multiple_of((i // (both // seq)) * tn, tn)
            o = acc[pl.ds(m, seq), pl.ds(c, tn)]
            p = (
                acc[pl.ds(both + m, seq), pl.ds(c, tn)]
                * own[i // (both // seq), pl.ds(m, seq), :]
            )
            place = lax.broadcasted_iota(jnp.int32, p.shape, 0)
            before = jnp.where(place > 0, pltpu.roll(p, 1, 0), 0.0)
            after = jnp.where(place < seq - 1, pltpu.roll(p, seq - 1, 0), 0.0)
            taps = taps_ref[:, pl.ds(c, tn)]
            conv = taps[0:1] * before + taps[1:2] * p + taps[2:3] * after
            mixed[pl.ds(m, seq), pl.ds(c, tn)] = (o * conv).astype(BF)
            return 0

        lax.fori_loop(0, (both // seq) * (wch // tn), unit, 0)

    def norm(base_ref, terms, gain_ref, dest_ref, start, count):
        tm = 32

        def unit(i, _):
            m = pl.multiple_of(start + i * tm, tm)
            parts = []
            for b in range(n):
                part = (
                    residual_scale
                    * base_ref[pl.ds(m, tm), pl.ds(b * nc, nc)].astype(F32)
                    + own[b, pl.ds(m, tm)]
                )
                for term in terms:
                    part = part + term[b, pl.ds(m, tm)].astype(F32)
                parts.append(part)
            total = parts[0]
            for b in range(1, n):
                total = total + parts[b]
            mean = jnp.sum(total, axis=-1, keepdims=True) / d
            parts = [p - mean for p in parts]
            square = parts[0] * parts[0]
            for b in range(1, n):
                square = square + parts[b] * parts[b]
            spread = jnp.sum(square, axis=-1, keepdims=True) / d
            scale = lax.rsqrt(spread + norm_epsilon)
            for b in range(n):
                cols = pl.ds(b * nc, nc)
                dest_ref[pl.ds(m, tm), cols] = (
                    parts[b] * scale * gain_ref[:, cols]
                ).astype(BF)
            return 0

        lax.fori_loop(0, count // tm, unit, 0)

    def near_first(p):
        return mate_copy(
            first_sem + p, fst.at[pl.ds(p * pr, pr)], fst.at[pl.ds(MATE + p * pr, pr)]
        )

    def twin_first(p):
        return across_copy(
            p, fst.at[pl.ds(p * pr, pr)], fst.at[pl.ds(TWIN + p * pr, pr)]
        )

    def diag_first(p):
        return mate_copy(
            diag_sem + p,
            fst.at[pl.ds(TWIN + p * pr, pr)],
            fst.at[pl.ds(DIAG + p * pr, pr)],
        )

    def make_first():
        for k, o in every:
            mix_block(k, o).wait_recv()
        for p in range(pieces):
            norm(tok, (precv1,), norm1_ref, fst, p * pr, pr)
            twin_first(p).start()
            near_first(p).start()

    def take_near():
        for p in range(pieces):
            near_first(p).wait_recv()

    def relay_first(p):
        twin_first(p).wait_recv()
        diag_first(p).start()

    def take_far(p, count):
        for q in range(p, p + count):
            diag_first(q).wait_recv()

    def free_sends():
        for k, o in every:
            mix_block(k, o).wait_send()

    plan = {}

    def after(ti, h, which, *work):
        plan.setdefault((ti, h, which), []).extend(work)

    def project_at(h):
        def work():
            if h:
                arrived(0, h)
            project(h)

        return work

    def mixout_at(h):
        def work():
            if h:
                arrived(1, h)
            mixout(h)

        return work

    def do(function, *values):
        return lambda: function(*values)

    last = half - 1
    until = list(range(half))
    most = pieces - 1
    after(0, 1, 0, project_at(0))
    for h in range(1, last):
        after(0, h + 1, 1, project_at(h))
    after(1, 1, 0, do(arrived, 0, last), do(project, last, (0,)))
    after(1, 1, 1, do(project, last, (1,)))
    after(1, 2, 0, do(project, last, (2,)))
    after(1, 2, 1, project_at(half))
    after(1, last, 0, mix)
    for h in range(half + 1):
        after(1, *((last, 1) if h < last - 1 else (half, 0)), mixout_at(h))
    after(1, half, 0, make_first)
    after(2, 1, 0, take_near, do(raise_near, 0))
    for h in range(1, half):
        after(2, h, 1, do(raise_near, h))
    after(2, 2, 0, do(relay_first, 0))
    after(2, 2, 1, do(relay_first, 1))
    for p in range(2, most):
        after(2, last, 1, do(relay_first, p))
    after(2, last, 1, do(take_far, 0, most), do(raise_far, 0, most, until))
    after(2, half, 0, do(relay_first, most))
    after(2, half, 0, do(raise_far, 0, most, [half]), do(take_far, most, 1))
    after(2, half, 0, do(raise_far, most, 1, until + [half]))
    after(2, half, 0, do(lower_far, 0), do(raise_near, half), do(pass_across, 0))
    after(3, 1, 0, free_sends)
    for h in range(1, half):
        after(3, h, 1, do(lower_far, h), do(lower_near, h - 1), do(pass_across, h))
    after(3, half, 0, do(lower_far, half), do(lower_near, half - 1))
    after(3, half, 0, do(pass_across, half), do(lower_near, half))

    for ti in range(4):
        for e in events(ti):
            event(*e)
            for work in plan.get(e, ()):
                work()

    for k, o in every:
        near_block(k, o).wait_recv()
    for k, o in every:
        across_block(k, o).wait_recv()
    norm(fst, (precv2, xrecv), norm2_ref, out_ref, 0, rows)

    for k, o in every:
        near_block(k, o).wait_send()
        far_block(k, o).wait_send()
        across_block(k, o).wait_send()
    for p in range(pieces):
        near_first(p).wait_send()
        twin_first(p).wait_send()
        diag_first(p).wait_send()
    share.wait_send()
    for key in copies:
        copies[key].wait_send()


def fits(mesh, args):
    n = mesh.shape["fs"]
    rows, d = args[0].shape
    ks, wch = args[1].shape
    nc = args[5].shape[1]
    ff = args[7].shape[1] // 2
    return (
        mesh.shape["rep"] == 2
        and mesh.shape["tp"] == 2
        and n % 2 == 0
        and n >= 8
        and ks % 128 == 0
        and nc == 256
        and wch % 256 == 0
        and ff % 256 == 0
        and wch // 256 <= n
        and wch <= 2 * rows
        and ff <= 4 * rows
        and ks <= rows
        and rows % SEQ == 0
        and rows % 128 == 0
    )


def fused(mesh, *args):
    (
        tokens,
        outer_weight,
        inner_weight,
        value_weight,
        conv_taps,
        mix_out,
        norm_first,
        up_weight,
        down_weight,
        norm_second,
    ) = args
    n = mesh.shape["fs"]
    rows, d = tokens.shape
    ks, wch = outer_weight.shape
    ff = up_weight.shape[1] // 2
    nc = mix_out.shape[1]
    both = 2 * rows
    anywhere = pl.BlockSpec(memory_space=pl.ANY)
    vmem = pl.BlockSpec(memory_space=pltpu.VMEM)
    messages = 4 * (3 * n - 3)
    pairs = 9 + 3 * n
    return pl.pallas_call(
        functools.partial(layer_kernel, n),
        out_shape=jax.ShapeDtypeStruct((rows, d), BF),
        in_specs=[
            anywhere,
            anywhere,
            anywhere,
            anywhere,
            vmem,
            anywhere,
            vmem,
            anywhere,
            anywhere,
            vmem,
        ],
        out_specs=vmem,
        scratch_shapes=[
            pltpu.VMEM((3, n, ks, wch), BF),
            pltpu.VMEM((n, wch, nc), BF),
            pltpu.VMEM((n * ks, ff), BF),
            pltpu.VMEM((n, ff, nc), BF),
            pltpu.VMEM((both, d), BF),
            pltpu.VMEM((2 * both, max(wch, ff)), F32),
            pltpu.VMEM((both, wch), BF),
            pltpu.VMEM((n, both, nc), F32),
            pltpu.VMEM((n, both, nc), BF),
            pltpu.VMEM((n, rows, nc), BF),
            pltpu.VMEM((n, both, nc), BF),
            pltpu.VMEM((n, rows, nc), BF),
            pltpu.VMEM((n, rows, nc), BF),
            pltpu.VMEM((2 * both, d), BF),
            pltpu.VMEM((2 * both, ff), BF),
            pltpu.SemaphoreType.DMA((8,)),
            pltpu.SemaphoreType.DMA((messages,)),
            pltpu.SemaphoreType.DMA((messages,)),
            pltpu.SemaphoreType.DMA((pairs,)),
            pltpu.SemaphoreType.DMA((pairs,)),
            pltpu.SemaphoreType.DMA((4 + n,)),
            pltpu.SemaphoreType.DMA((4 + n,)),
        ],
        compiler_params=pltpu.CompilerParams(
            collective_id=0, has_side_effects=True, vmem_limit_bytes=67043328
        ),
        name="layer",
    )(
        tokens,
        outer_weight,
        inner_weight,
        value_weight,
        conv_taps,
        mix_out,
        norm_first.reshape(1, d),
        up_weight,
        down_weight,
        norm_second.reshape(1, d),
    )


def solution(mesh):
    def body(*args):
        return fused(mesh, *args) if fits(mesh, args) else local(*args)

    return jax.shard_map(
        body,
        mesh=mesh,
        in_specs=(
            P(("rep", "fs", "tp"), None),
            P("fs", "tp"),
            P("fs", "tp"),
            P("fs", "tp"),
            P(None, "tp"),
            P("tp", "fs"),
            P(),
            P("fs", "tp"),
            P("tp", "fs"),
            P(),
        ),
        out_specs=P(("rep", "fs", "tp"), None),
        check_vma=False,
    )
```
